32 devices in a mesh: sp: 4 (over z), fs: 4 (over y, x), tp: 2 (over core).
Axes of the slice: x: 2, y: 2, z: 4, core: 2. Of those that a mesh axis runs over, the one named last changes fastest.
Arguments:
- tokens: bfloat16 [2048, 2048], P('sp', ('fs', 'tp')), may hold values from -6 to 6
- in_gain: float32 [2048], replicated, may hold values from 0.1 to 1.9
- conv_a_weight: bfloat16 [2048, 1024], P(None, ('fs', 'tp')), may hold values from -0.125 to 0.125
- conv_gate_weight: bfloat16 [2048, 1024], P(None, ('fs', 'tp')), may hold values from -0.125 to 0.125
- query_weight: bfloat16 [2048, 1024], P(None, ('fs', 'tp')), may hold values from -0.125 to 0.125
- key_weight: bfloat16 [2048, 1024], P(None, ('fs', 'tp')), may hold values from -0.125 to 0.125
- value_weight: bfloat16 [2048, 1024], P(None, ('fs', 'tp')), may hold values from -0.125 to 0.125
- conv_taps: bfloat16 [31, 1024], replicated, may hold values from -3 to 3
- conv_norm_gain: float32 [1024], replicated, may hold values from 0.1 to 1.9
- break_shift: bfloat16 [16, 2048], P(('fs', 'tp'), 'sp'), may hold values from -20 to 1
- conv_out_gain: float32 [1024], replicated, may hold values from 0.1 to 1.9
- attn_out_gain: float32 [1024], replicated, may hold values from 0.1 to 1.9
- out_weight: bfloat16 [2048, 2048], P(None, ('fs', 'tp')), may hold values from -0.125 to 0.125
Outputs:
- mixed: bfloat16 [2048, 2048], P('sp', ('fs', 'tp'))
The draws below stay inside these ranges and needn't reach their ends.
All inputs are finite; a program needn't handle non-finite values.
Results may differ from the reference program's by a relative error of at most 0.0078.
Values may be sent and summed in bfloat16 or wider, within the bound.
A program may use at most 128 MiB of HBM per device.

```python
import math
import jax
import jax.numpy as jnp
from jax import lax

D = 2048
HEAD_DIM = 64
KERNEL = 31
TOK_DEV = 512
SEQUENCE_TOKENS = 2048
CONV_CH = 1024
SB_WIDTH = 1024
HEADS = 16


def draw_conv_taps(key, part):
    columns = jnp.arange(D // 2, dtype=jnp.float32) / (D // 2)
    entries = jnp.clip(jax.random.normal(key, (KERNEL, D // 2), jnp.float32), -4.0, 4.0)
    rising = 1.0 + 2.0 * columns
    return (entries * rising[None, :] * KERNEL ** (-0.5)).astype(jnp.bfloat16)


def draw_break_shift(key, part):
    key_sequence = jax.random.split(key, 5)
    count_of_heads = D // 2 // HEAD_DIM
    block_count = SEQUENCE_TOKENS // TOK_DEV
    slow_share = 0.5
    slow_heads = jax.random.uniform(key_sequence[0], (count_of_heads,), jnp.float32) < slow_share
    far_level = -math.log(SEQUENCE_TOKENS) - 0.5
    depth_tier = jnp.where(slow_heads, far_level, -3.0)
    block_factor = jnp.log(jax.random.uniform(key_sequence[1], (count_of_heads, block_count), jnp.float32, 0.5, 2.0))
    block_summand = jnp.repeat(block_factor, TOK_DEV, axis=1)
    coarse_estimate = jnp.clip(jax.random.normal(key_sequence[2], (count_of_heads, SEQUENCE_TOKENS), jnp.float32), -2.0, 2.0) * 0.5
    surge_groups = jax.random.uniform(key_sequence[3], (count_of_heads, SEQUENCE_TOKENS), jnp.float32) < 4.0 / SEQUENCE_TOKENS
    surge_depth = jax.random.uniform(key_sequence[4], (count_of_heads, SEQUENCE_TOKENS), jnp.float32, -1.5, 0.0)
    displaced_rows = jnp.where(surge_groups, surge_depth, depth_tier[:, None] + block_summand + coarse_estimate)
    return displaced_rows.astype(jnp.bfloat16)


def block_levels(own_key, extent, cuts, smallest, high):
    loudness = 1.0
    for dim, shards_of in cuts:
        heights = jax.random.uniform(jax.random.fold_in(jax.random.fold_in(own_key, 6), dim), (shards_of,), jnp.float32, smallest / len(cuts), high / len(cuts))
        loudness = loudness * jnp.repeat(jnp.exp(heights), extent[dim] // shards_of).reshape((-1,) + (1,) * (len(extent) - 1 - dim))
    return loudness


def bell_draw(key, extent, width, reach, cuts=(), kind=jnp.bfloat16):
    result = width * jax.random.normal(key, extent, jnp.float32)
    if cuts:
        result = result * block_levels(key, extent, cuts, -0.22, 0.18)
    return jnp.clip(result, -reach, reach).astype(kind)


def setup_inputs(seed: int = 0) -> dict:
    keys = jax.random.split(jax.random.key(seed), 14)
    return {
        "tokens": bell_draw(keys[0], (SEQUENCE_TOKENS, D), 1.0, 6.0, ((0, 4), (1, 8))),
        "in_gain": jnp.clip(1.0 + 0.18 * jax.random.normal(keys[1], (D,), jnp.float32), 0.1, 1.9),
        "conv_a_weight": bell_draw(keys[2], (D, CONV_CH), D ** -0.5, 0.125, ((1, 8),)),
        "conv_gate_weight": bell_draw(keys[3], (D, CONV_CH), D ** -0.5, 0.125, ((1, 8),)),
        "query_weight": bell_draw(keys[4], (D, SB_WIDTH), D ** -0.5, 0.125, ((1, 8),)),
        "key_weight": bell_draw(keys[5], (D, SB_WIDTH), D ** -0.5, 0.125, ((1, 8),)),
        "value_weight": bell_draw(keys[6], (D, SB_WIDTH), D ** -0.5, 0.125, ((1, 8),)),
        "conv_taps": draw_conv_taps(jax.random.fold_in(keys[13], 71), 0),
        "conv_norm_gain": jnp.clip(1.0 + 0.18 * jax.random.normal(keys[8], (CONV_CH,), jnp.float32), 0.1, 1.9),
        "break_shift": draw_break_shift(jax.random.fold_in(keys[13], 71), 0),
        "conv_out_gain": jnp.clip(1.0 + 0.18 * jax.random.normal(keys[10], (CONV_CH,), jnp.float32), 0.1, 1.9),
        "attn_out_gain": jnp.clip(1.0 + 0.18 * jax.random.normal(keys[11], (SB_WIDTH,), jnp.float32), 0.1, 1.9),
        "out_weight": bell_draw(keys[12], (D, D), D ** -0.5, 0.125, ((1, 8),)),
    }


epsilon = 1e-06

def project_rows(scaled_input, weight, input_scale):
    product = jnp.dot(scaled_input, weight, preferred_element_type=jnp.float32)
    return (product * input_scale).astype(jnp.bfloat16)

def branch_output(mixed_part, gain, rows):
    mixed_wide = mixed_part.astype(jnp.float32)
    branch_scale = lax.rsqrt(lax.optimization_barrier(jnp.mean(mixed_wide * mixed_wide, axis=1, keepdims=True)) + epsilon)
    scaled = (mixed_wide * gain[None, :]).astype(jnp.bfloat16)
    return jnp.dot(scaled, rows, preferred_element_type=jnp.float32) * branch_scale

def reference(tokens, in_gain, conv_a_weight, conv_gate_weight, query_weight, key_weight, value_weight, conv_taps, conv_norm_gain, break_shift, conv_out_gain, attn_out_gain, out_weight):
    tokens_wide = tokens.astype(jnp.float32)
    input_scale = lax.rsqrt(lax.optimization_barrier(jnp.mean(tokens_wide * tokens_wide, axis=1, keepdims=True)) + epsilon)
    scaled_input = (tokens_wide * in_gain[None, :]).astype(jnp.bfloat16)
    conv_a = project_rows(scaled_input, conv_a_weight, input_scale)
    conv_gate = project_rows(scaled_input, conv_gate_weight, input_scale)
    query = project_rows(scaled_input, query_weight, input_scale)
    key = project_rows(scaled_input, key_weight, input_scale)
    value = project_rows(scaled_input, value_weight, input_scale)
    gated_input = conv_a.astype(jnp.float32) * jax.nn.sigmoid(conv_gate.astype(jnp.float32))
    padded = jnp.pad(gated_input, ((KERNEL - 1, 0), (0, 0)))
    tap_values = conv_taps.astype(jnp.float32)
    conv_out = jnp.zeros((SEQUENCE_TOKENS, CONV_CH), jnp.float32)
    for offset in range(KERNEL):
        conv_out = conv_out + tap_values[offset][None, :] * padded[offset:offset + SEQUENCE_TOKENS]
    row_mean = lax.optimization_barrier(jnp.mean(conv_out, axis=1, keepdims=True))
    centered = conv_out - row_mean
    row_spread = lax.optimization_barrier(jnp.mean(centered * centered, axis=1, keepdims=True))
    normed = centered * lax.rsqrt(row_spread + epsilon) * conv_norm_gain[None, :]
    conv_mixed = jax.nn.silu(normed).astype(jnp.bfloat16)
    query_heads = query.astype(jnp.float32).reshape(SEQUENCE_TOKENS, HEADS, HEAD_DIM)
    key_heads = key.astype(jnp.float32).reshape(SEQUENCE_TOKENS, HEADS, HEAD_DIM)
    value_heads = value.astype(jnp.float32).reshape(SEQUENCE_TOKENS, HEADS, HEAD_DIM)
    shifts = break_shift.astype(jnp.float32)
    score_scale = HEAD_DIM ** (-0.5)
    block_count = SEQUENCE_TOKENS // TOK_DEV

    def one_block(block_index):
        first_query = (block_index * TOK_DEV).astype(jnp.int32)
        queries = lax.dynamic_slice_in_dim(query_heads, first_query, TOK_DEV, 0)
        query_pos = first_query + jnp.arange(TOK_DEV, dtype=jnp.int32)

        def advance(counter, running):
            outputs, behind = running
            begin_row = ((block_index - counter) * TOK_DEV).astype(jnp.int32)
            key_rows = lax.dynamic_slice_in_dim(key_heads, begin_row, TOK_DEV, 0)
            value_rows = lax.dynamic_slice_in_dim(value_heads, begin_row, TOK_DEV, 0)
            shift_rows = lax.dynamic_slice_in_dim(shifts, begin_row, TOK_DEV, 1)
            scores = jnp.einsum('qhd,khd->hqk', queries, key_rows) * score_scale
            scores = scores + shift_rows[:, None, :]
            key_pos = begin_row + jnp.arange(TOK_DEV, dtype=jnp.int32)
            allowed = (key_pos[None, :] < query_pos[:, None])[None]
            log_fail = jnp.where(allowed, jax.nn.log_sigmoid(-scores), 0.0)
            later_sum = lax.cumsum(log_fail, axis=2, reverse=True) - log_fail + behind[:, :, None]
            weights = jnp.where(allowed, jnp.exp(jax.nn.log_sigmoid(scores) + later_sum), 0.0).astype(jnp.bfloat16)
            weights = lax.optimization_barrier(weights).astype(jnp.float32)
            outputs = outputs + jnp.einsum('hqk,khd->qhd', weights, value_rows)
            return (outputs, behind + lax.optimization_barrier(jnp.sum(log_fail, axis=2)))
        start_state = (jnp.zeros((TOK_DEV, HEADS, HEAD_DIM), jnp.float32), jnp.zeros((HEADS, TOK_DEV), jnp.float32))
        outputs, behind = lax.fori_loop(0, block_index + 1, advance, start_state)
        return outputs
    blocks_out = lax.map(one_block, jnp.arange(block_count, dtype=jnp.int32))
    attn_mixed = blocks_out.reshape(SEQUENCE_TOKENS, SB_WIDTH).astype(jnp.bfloat16)
    total = branch_output(conv_mixed, conv_out_gain, out_weight[:CONV_CH])
    total = total + branch_output(attn_mixed, attn_out_gain, out_weight[CONV_CH:])
    return total.astype(jnp.bfloat16)
```

```python
import functools
import math

import jax
import jax.numpy as jnp
from jax import lax
from jax.experimental import pallas as pl
from jax.experimental.pallas import tpu as pltpu
from jax.sharding import PartitionSpec as P

HEAD_DIM = 64
LANES = 128
KEY_TILE = 256
HALO = 32
LOG2E = math.log2(math.e)
MESH = pl.DeviceIdType.MESH
F32 = jnp.float32
BF16 = jnp.bfloat16

epsilon = 1e-06


def dot_tt(left, right, precision=None):
    return lax.dot_general(
        left, right, (((1,), (1,)), ((), ())), precision=precision, preferred_element_type=F32
    )


def layer_kernel(
    nsp,
    nfs,
    ntp,
    tokens,
    w_a,
    w_gate,
    w_q,
    w_k,
    w_v,
    w_out,
    in_gain,
    taps,
    norm_gain,
    shift,
    conv_gain,
    attn_gain,
    out,
    xbuf,
    wbuf,
    wout,
    acc,
    squares,
    qbuf,
    kvbuf,
    shbuf,
    gbuf,
    convbuf,
    tri,
    stat,
    own_conv,
    own_attn,
    cbuf,
    abuf,
    obuf,
    behind,
    local_sem,
    tok_send,
    tok_recv,
    tokp_send,
    tokp_recv,
    att_send,
    att_recv,
    attp_send,
    attp_recv,
    kv_send,
    kv_recv,
    sh_send,
    sh_recv,
    halo_sem,
    stat_send,
    stat_recv,
    conv_send,
    conv_recv,
):
    s = lax.axis_index("sp")
    f = lax.axis_index("fs")
    c = lax.axis_index("tp")
    group = nfs * ntp
    g = f * ntp + c
    rows = tokens.shape[0]
    cols = tokens.shape[1]
    width = w_a.shape[1]
    heads = shift.shape[0]
    channels = width * group
    model = cols * group

    def in_group(index):
        return {"fs": index // ntp, "tp": lax.rem(index, ntp)}

    barrier = pltpu.get_barrier_semaphore()
    for d in range(1, group):
        pl.semaphore_signal(
            barrier, inc=1, device_id=in_group(lax.rem(g + d, group)), device_id_type=MESH
        )

    def greet(d, carry):
        pl.semaphore_signal(
            barrier, inc=1, device_id={"sp": lax.rem(s + d, nsp)}, device_id_type=MESH
        )
        return carry

    lax.fori_loop(1, nsp, greet, 0)

    locals_ = [pltpu.make_async_copy(tokens, xbuf.at[g], local_sem.at[0])]
    for i, w in enumerate((w_a, w_gate, w_q, w_k, w_v)):
        locals_.append(
            pltpu.make_async_copy(
                w, wbuf.at[:, pl.ds(i * width, width)], local_sem.at[1 + i]
            )
        )
    locals_.append(pltpu.make_async_copy(w_out, wout, local_sem.at[6]))
    for copy in locals_:
        copy.start()

    shbuf[0] = jnp.zeros(shbuf.shape[1:], F32)
    shbuf[0, pl.ds(0, heads), :] = shift[...].astype(F32) * LOG2E
    ki = lax.broadcasted_iota(jnp.int32, (KEY_TILE, KEY_TILE), 0)
    kj = lax.broadcasted_iota(jnp.int32, (KEY_TILE, KEY_TILE), 1)
    tri[...] = (ki >= kj).astype(F32).astype(BF16)

    pl.semaphore_wait(barrier, group - 1 + nsp - 1)

    def direct(src, dst, send, recv, k):
        return pltpu.make_async_remote_copy(
            src_ref=src,
            dst_ref=dst,
            send_sem=send.at[k],
            recv_sem=recv.at[k],
            device_id={"fs": lax.rem(f + k, nfs)},
            device_id_type=MESH,
        )

    def partner(src, dst, send, recv, m, k):
        return pltpu.make_async_remote_copy(
            src_ref=src,
            dst_ref=dst,
            send_sem=send.at[m, k],
            recv_sem=recv.at[m, k],
            device_id={"tp": lax.rem(c + m, ntp)},
            device_id_type=MESH,
        )

    def chip_from(k):
        return lax.rem(f + nfs - k, nfs)

    def gather(own, buf, sems, consume):
        send, recv, psend, precv = sems
        sent = []
        for k in range(1, nfs):
            copy = direct(own, buf.at[g], send, recv, k)
            copy.start()
            sent.append(copy)
        for m in range(1, ntp):
            copy = partner(own, buf.at[g], psend, precv, m, 0)
            copy.start()
            sent.append(copy)
        consume(g, True)
        for m in range(1, ntp):
            origin = f * ntp + lax.rem(c + ntp - m, ntp)
            partner(own, buf.at[origin], psend, precv, m, 0).wait_recv()
            consume(origin, False)
        for k in range(1, nfs):
            origin = chip_from(k) * ntp + c
            direct(own, buf.at[origin], send, recv, k).wait_recv()
            for m in range(1, ntp):
                copy = partner(buf.at[origin], buf.at[origin], psend, precv, m, k)
                copy.start()
                sent.append(copy)
            consume(origin, False)
        for k in range(1, nfs):
            for m in range(1, ntp):
                origin = chip_from(k) * ntp + lax.rem(c + ntp - m, ntp)
                partner(own, buf.at[origin], psend, precv, m, k).wait_recv()
                consume(origin, False)
        return sent

    def send_shift(d, carry):
        pltpu.make_async_remote_copy(
            src_ref=shbuf.at[0],
            dst_ref=shbuf.at[d],
            send_sem=sh_send.at[d],
            recv_sem=sh_recv.at[d],
            device_id={"sp": s + d},
            device_id_type=MESH,
        ).start()
        return carry

    def project(index, first):
        if first:
            for copy in locals_[:6]:
                copy.wait()
        x = xbuf[index].astype(F32)
        per = cols // LANES
        gain = jnp.concatenate(
            [in_gain[pl.ds(index * per + j, 1), :] for j in range(per)], axis=1
        )
        scaled = (x * gain).astype(BF16)
        w = wbuf[pl.ds(pl.multiple_of(index * cols, cols), cols), :]
        part = jnp.dot(scaled, w, preferred_element_type=F32)
        sq = x * x
        folded = sq[:, :LANES]
        for j in range(1, per):
            folded = folded + sq[:, j * LANES : (j + 1) * LANES]
        if first:
            acc[...] = part
            squares[...] = folded
        else:
            acc[...] += part
            squares[...] += folded

    sent = gather(tokens, xbuf, (tok_send, tok_recv, tokp_send, tokp_recv), project)
    lax.fori_loop(1, nsp - s, send_shift, 0)

    scale = lax.rsqrt(jnp.sum(squares[...], axis=1, keepdims=True) / model + epsilon)

    def projected(i):
        return (acc[:, i * width : (i + 1) * width] * scale).astype(BF16)

    kvbuf[0, :, :width] = projected(3)
    kvbuf[0, :, width:] = projected(4)

    a = projected(0).astype(F32)
    gate = projected(1).astype(F32)
    gbuf[pl.ds(HALO, rows), :] = a / (1.0 + jnp.exp(-gate))

    def kv_copy(d):
        return pltpu.make_async_remote_copy(
            src_ref=kvbuf.at[0],
            dst_ref=kvbuf.at[d],
            send_sem=kv_send.at[d],
            recv_sem=kv_recv.at[d],
            device_id={"sp": lax.rem(s + d, nsp)},
            device_id_type=MESH,
        )

    def sh_copy(d):
        return pltpu.make_async_remote_copy(
            src_ref=shbuf.at[0],
            dst_ref=shbuf.at[d],
            send_sem=sh_send.at[d],
            recv_sem=sh_recv.at[d],
            device_id={"sp": lax.rem(s + d, nsp)},
            device_id_type=MESH,
        )

    halo = pltpu.make_async_remote_copy(
        src_ref=gbuf.at[pl.ds(rows, HALO)],
        dst_ref=gbuf.at[pl.ds(0, HALO)],
        send_sem=halo_sem.at[0],
        recv_sem=halo_sem.at[1],
        device_id={"sp": lax.rem(s + 1, nsp)},
        device_id_type=MESH,
    )

    @pl.when(s + 1 < nsp)
    def _():
        halo.start()

    def send_kv(d, carry):
        kv_copy(d).start()
        return carry

    lax.fori_loop(1, nsp - s, send_kv, 0)

    lane = lax.broadcasted_iota(jnp.int32, (1, width), 1)
    head_lanes = [
        ((lane >= h * HEAD_DIM) & (lane < (h + 1) * HEAD_DIM)).astype(F32) for h in range(heads)
    ]
    q = projected(2).astype(F32) * (HEAD_DIM**-0.5)
    for h in range(heads):
        qbuf[h] = (q * head_lanes[h]).astype(BF16)
    obuf[...] = jnp.zeros_like(obuf)
    behind[...] = jnp.zeros_like(behind)

    def tile(slot, h, row0, count, key0, masked):
        rs = pl.ds(row0, count)
        keys = kvbuf[slot, pl.ds(key0, KEY_TILE), :width]
        values = kvbuf[slot, pl.ds(key0, KEY_TILE), width:]
        values = (values.astype(F32) * head_lanes[h]).astype(BF16)
        shifts = shbuf[slot, pl.ds(h, 1), pl.ds(key0, KEY_TILE)]
        scores = dot_tt(qbuf[h, rs, :], keys) * LOG2E + shifts
        fail = jnp.maximum(scores, 0.0) + LOG2E * jnp.log(1.0 + jnp.exp2(-jnp.abs(scores)))
        if masked:
            qi = row0 + lax.broadcasted_iota(jnp.int32, (count, KEY_TILE), 0)
            kk = key0 + lax.broadcasted_iota(jnp.int32, (count, KEY_TILE), 1)
            allowed = kk < qi
            fail = jnp.where(allowed, fail, 0.0)
        high = fail.astype(BF16)
        low = (fail - high.astype(F32)).astype(BF16)
        sums = jnp.dot(high, tri[...], preferred_element_type=F32) + jnp.dot(
            low, tri[...], preferred_element_type=F32
        )
        past = behind[h, rs, :]
        past_wide = jnp.concatenate([past] * (KEY_TILE // LANES), axis=1)
        weights = jnp.exp2(scores - sums - past_wide)
        if masked:
            weights = jnp.where(allowed, weights, 0.0)
        obuf[rs, :] += jnp.dot(weights.astype(BF16), values, preferred_element_type=F32)
        behind[h, rs, :] = past + sums[:, :1]

    tiles = rows // KEY_TILE
    for h in range(heads):
        for qt in range(tiles):
            for kt in range(qt, -1, -1):
                tile(0, h, qt * KEY_TILE, KEY_TILE, kt * KEY_TILE, kt == qt)

    @pl.when(s == 0)
    def _():
        gbuf[pl.ds(0, HALO), :] = jnp.zeros((HALO, width), F32)

    @pl.when(s > 0)
    def _():
        halo.wait_recv()

    ntaps = taps.shape[0]
    tap = taps[:, pl.ds(pl.multiple_of(g * width, width), width)].astype(F32)
    chunk = 128
    for r0 in range(0, rows, chunk):
        total = jnp.zeros((chunk, width), F32)
        for j in range(ntaps):
            first = r0 + j + HALO - (ntaps - 1)
            total = total + tap[j : j + 1, :] * gbuf[pl.ds(first, chunk), :]
        convbuf[pl.ds(r0, chunk), :] = total

    conv = convbuf[...]
    ones = jnp.ones((8, width), F32)
    sub = lax.broadcasted_iota(jnp.int32, (8, rows), 0)
    hp = lax.Precision.HIGHEST
    stat[0] = jnp.where(sub == 0, dot_tt(ones, conv, hp), dot_tt(ones, conv * conv, hp))

    def stat_copy(d):
        return pltpu.make_async_remote_copy(
            src_ref=stat.at[0],
            dst_ref=stat.at[d],
            send_sem=stat_send.at[d],
            recv_sem=stat_recv.at[d],
            device_id=in_group(lax.rem(g + d, group)),
            device_id_type=MESH,
        )

    for d in range(1, group):
        stat_copy(d).start()
    totals = stat[0]
    for d in range(1, group):
        stat_copy(d).wait_recv()
        totals = totals + stat[d]
    pick = lax.broadcasted_iota(jnp.int32, (8, width), 0)
    turned = (((0,), (0,)), ((), ()))
    first_sum = lax.dot_general(
        totals, (pick == 0).astype(F32), turned, precision=hp, preferred_element_type=F32
    )
    second_sum = lax.dot_general(
        totals, (pick == 1).astype(F32), turned, precision=hp, preferred_element_type=F32
    )
    mean = first_sum / channels
    spread = jnp.maximum(second_sum / channels - mean * mean, 0.0)
    normed = (conv - mean) * lax.rsqrt(spread + epsilon) * norm_gain[pl.ds(g, 1), :]
    mixed = (normed / (1.0 + jnp.exp(-normed))).astype(BF16)
    own_conv[...] = mixed
    cbuf[g] = mixed

    def conv_copy(d, index):
        return pltpu.make_async_remote_copy(
            src_ref=own_conv,
            dst_ref=cbuf.at[index],
            send_sem=conv_send.at[d],
            recv_sem=conv_recv.at[d],
            device_id=in_group(lax.rem(g + d, group)),
            device_id_type=MESH,
        )

    for d in range(1, group):
        conv_copy(d, g).start()

    def attend(d, carry):
        sh_copy(d).wait_recv()
        kv_copy(d).wait_recv()
        for h in range(heads):
            for kt in range(tiles - 1, -1, -1):
                tile(d, h, 0, rows, kt * KEY_TILE, False)
        return carry

    lax.fori_loop(1, s + 1, attend, 0)

    attn = obuf[...].astype(BF16)
    own_attn[...] = attn
    abuf[g] = attn

    locals_[6].wait()

    def mix(buf, gain, base, index, first):
        v = buf[index].astype(F32)
        scaled = (v * gain[pl.ds(index, 1), :]).astype(BF16)
        w = wout[pl.ds(pl.multiple_of(base + index * width, width), width), :]
        part = jnp.dot(scaled, w, preferred_element_type=F32)
        if first:
            acc[:, : out.shape[1]] = part
            squares[...] = v * v
        else:
            acc[:, : out.shape[1]] += part
            squares[...] += v * v

    def mix_conv():
        mix(cbuf, conv_gain, 0, g, True)
        for d in range(1, group):
            origin = lax.rem(g + group - d, group)
            conv_copy(d, origin).wait_recv()
            mix(cbuf, conv_gain, 0, origin, False)
        conv_scale = lax.rsqrt(
            jnp.sum(squares[...], axis=1, keepdims=True) / channels + epsilon
        )
        out_width = out.shape[1]
        acc[:, out_width : 2 * out_width] = acc[:, :out_width] * conv_scale

    def mix_attn(index, first):
        if first:
            mix_conv()
        mix(abuf, attn_gain, channels, index, first)

    sent += gather(own_attn, abuf, (att_send, att_recv, attp_send, attp_recv), mix_attn)
    out_width = out.shape[1]
    attn_scale = lax.rsqrt(jnp.sum(squares[...], axis=1, keepdims=True) / channels + epsilon)
    out[...] = (acc[:, out_width : 2 * out_width] + acc[:, :out_width] * attn_scale).astype(BF16)

    for copy in sent:
        copy.wait_send()
    for d in range(1, group):
        stat_copy(d).wait_send()
        conv_copy(d, g).wait_send()

    @pl.when(s + 1 < nsp)
    def _():
        halo.wait_send()

    def finish(d, carry):
        sh_copy(d).wait_send()
        kv_copy(d).wait_send()
        return carry

    lax.fori_loop(1, nsp - s, finish, 0)


def per_device(
    tokens,
    in_gain,
    conv_a_weight,
    conv_gate_weight,
    query_weight,
    key_weight,
    value_weight,
    conv_taps,
    conv_norm_gain,
    break_shift,
    conv_out_gain,
    attn_out_gain,
    out_weight,
):
    nsp, nfs, ntp = (lax.axis_size(axis) for axis in ("sp", "fs", "tp"))
    group = nfs * ntp
    rows, cols = tokens.shape
    model = in_gain.shape[0]
    width = conv_a_weight.shape[1]
    heads = break_shift.shape[0]
    out_width = out_weight.shape[1]
    vm = pl.BlockSpec(memory_space=pltpu.VMEM)
    hbm = pl.BlockSpec(memory_space=pl.ANY)
    dma = pltpu.SemaphoreType.DMA
    return pl.pallas_call(
        functools.partial(layer_kernel, nsp, nfs, ntp),
        out_shape=jax.ShapeDtypeStruct((rows, out_width), BF16),
        in_specs=[hbm] * 7 + [vm] * 6,
        out_specs=vm,
        scratch_shapes=[
            pltpu.VMEM((group, rows, cols), BF16),
            pltpu.VMEM((model, 5 * width), BF16),
            pltpu.VMEM((model, out_width), BF16),
            pltpu.VMEM((rows, 5 * width), F32),
            pltpu.VMEM((rows, LANES), F32),
            pltpu.VMEM((heads, rows, width), BF16),
            pltpu.VMEM((nsp, rows, 2 * width), BF16),
            pltpu.VMEM((nsp, 8, rows), F32),
            pltpu.VMEM((HALO + rows, width), F32),
            pltpu.VMEM((rows, width), F32),
            pltpu.VMEM((KEY_TILE, KEY_TILE), BF16),
            pltpu.VMEM((group, 8, rows), F32),
            pltpu.VMEM((rows, width), BF16),
            pltpu.VMEM((rows, width), BF16),
            pltpu.VMEM((group, rows, width), BF16),
            pltpu.VMEM((group, rows, width), BF16),
            pltpu.VMEM((rows, width), F32),
            pltpu.VMEM((heads, rows, LANES), F32),
            dma((7,)),
            dma((nfs,)),
            dma((nfs,)),
            dma((ntp, nfs)),
            dma((ntp, nfs)),
            dma((nfs,)),
            dma((nfs,)),
            dma((ntp, nfs)),
            dma((ntp, nfs)),
            dma((nsp,)),
            dma((nsp,)),
            dma((nsp,)),
            dma((nsp,)),
            dma((2,)),
            dma((group,)),
            dma((group,)),
            dma((group,)),
            dma((group,)),
        ],
        compiler_params=pltpu.CompilerParams(
            collective_id=0, has_side_effects=True, vmem_limit_bytes=48 * 2**20
        ),
        name="layer",
    )(
        tokens,
        conv_a_weight,
        conv_gate_weight,
        query_weight,
        key_weight,
        value_weight,
        out_weight,
        in_gain.reshape(-1, LANES),
        conv_taps,
        conv_norm_gain.reshape(-1, LANES),
        break_shift,
        conv_out_gain.reshape(-1, LANES),
        attn_out_gain.reshape(-1, LANES),
    )


def solution(mesh):
    split = P(None, ("fs", "tp"))
    return jax.shard_map(
        per_device,
        mesh=mesh,
        in_specs=(
            P("sp", ("fs", "tp")),
            P(),
            split,
            split,
            split,
            split,
            split,
            P(),
            P(),
            P(("fs", "tp"), "sp"),
            P(),
            P(),
            split,
        ),
        out_specs=P("sp", ("fs", "tp")),
        check_vma=False,
    )
```

```python
import functools
import math

import jax
import jax.numpy as jnp
from jax import lax
from jax.experimental import pallas as pl
from jax.experimental.pallas import tpu as pltpu
from jax.sharding import PartitionSpec as P

HEAD_DIM = 64
LANES = 128
KEY_TILE = 256
HALO = 32
LOG2E = math.log2(math.e)
MESH = pl.DeviceIdType.MESH
F32 = jnp.float32
BF16 = jnp.bfloat16

epsilon = 1e-06


def dot_tt(left, right, precision=None):
    return lax.dot_general(
        left, right, (((1,), (1,)), ((), ())), precision=precision, preferred_element_type=F32
    )


def layer_kernel(
    nsp,
    nfs,
    ntp,
    tokens,
    w_a,
    w_gate,
    w_q,
    w_k,
    w_v,
    w_out,
    in_gain,
    taps,
    norm_gain,
    shift,
    conv_gain,
    attn_gain,
    out,
    xbuf,
    wbuf,
    wout,
    acc,
    squares,
    qbuf,
    kvbuf,
    shbuf,
    gbuf,
    convbuf,
    tri,
    stat,
    own_conv,
    own_attn,
    cbuf,
    abuf,
    obuf,
    behind,
    local_sem,
    tok_send,
    tok_recv,
    tokp_send,
    tokp_recv,
    att_send,
    att_recv,
    attp_send,
    attp_recv,
    kv_send,
    kv_recv,
    sh_send,
    sh_recv,
    halo_sem,
    stat_send,
    stat_recv,
    conv_send,
    conv_recv,
    convp_send,
    convp_recv,
):
    s = lax.axis_index("sp")
    f = lax.axis_index("fs")
    c = lax.axis_index("tp")
    group = nfs * ntp
    g = f * ntp + c
    rows = tokens.shape[0]
    cols = tokens.shape[1]
    width = w_a.shape[1]
    heads = shift.shape[0]
    channels = width * group
    model = cols * group

    def in_group(index):
        return {"fs": index // ntp, "tp": lax.rem(index, ntp)}

    barrier = pltpu.get_barrier_semaphore()
    for d in range(1, group):
        pl.semaphore_signal(
            barrier, inc=1, device_id=in_group(lax.rem(g + d, group)), device_id_type=MESH
        )

    def greet(d, carry):
        pl.semaphore_signal(
            barrier, inc=1, device_id={"sp": lax.rem(s + d, nsp)}, device_id_type=MESH
        )
        return carry

    lax.fori_loop(1, nsp, greet, 0)

    locals_ = [pltpu.make_async_copy(tokens, xbuf.at[g], local_sem.at[0])]
    for i, w in enumerate((w_a, w_gate, w_q, w_k, w_v)):
        locals_.append(
            pltpu.make_async_copy(
                w, wbuf.at[:, pl.ds(i * width, width)], local_sem.at[1 + i]
            )
        )
    locals_.append(pltpu.make_async_copy(w_out, wout, local_sem.at[6]))
    for copy in locals_:
        copy.start()

    shbuf[0] = jnp.zeros(shbuf.shape[1:], F32)
    shbuf[0, pl.ds(0, heads), :] = shift[...].astype(F32) * LOG2E
    ki = lax.broadcasted_iota(jnp.int32, (KEY_TILE, KEY_TILE), 0)
    kj = lax.broadcasted_iota(jnp.int32, (KEY_TILE, KEY_TILE), 1)
    tri[...] = (ki >= kj).astype(F32).astype(BF16)

    pl.semaphore_wait(barrier, group - 1 + nsp - 1)

    def direct(src, dst, send, recv, k):
        return pltpu.make_async_remote_copy(
            src_ref=src,
            dst_ref=dst,
            send_sem=send,
            recv_sem=recv,
            device_id={"fs": lax.rem(f + k, nfs)},
            device_id_type=MESH,
        )

    def partner(src, dst, send, recv, m):
        return pltpu.make_async_remote_copy(
            src_ref=src,
            dst_ref=dst,
            send_sem=send,
            recv_sem=recv,
            device_id={"tp": lax.rem(c + m, ntp)},
            device_id_type=MESH,
        )

    def chip_from(k):
        return lax.rem(f + nfs - k, nfs)

    sent = []

    def start(own, view, sems, base):
        send, recv, psend, precv = sems
        for k in range(1, nfs):
            copy = direct(own, view(g), send.at[base + k], recv.at[base + k], k)
            copy.start()
            sent.append(copy)
        for m in range(1, ntp):
            copy = partner(own, view(g), psend.at[m, base], precv.at[m, base], m)
            copy.start()
            sent.append(copy)

    def relay(own, view, sems, base, consume):
        send, recv, psend, precv = sems
        for k in range(1, nfs):
            origin = chip_from(k) * ntp + c
            direct(own, view(origin), send.at[base + k], recv.at[base + k], k).wait_recv()
            for m in range(1, ntp):
                copy = partner(
                    view(origin), view(origin), psend.at[m, base + k], precv.at[m, base + k], m
                )
                copy.start()
                sent.append(copy)
            if consume is not None:
                consume(origin)

    def finish_relay(own, view, sems, base, consume):
        send, recv, psend, precv = sems
        for k in range(1, nfs):
            for m in range(1, ntp):
                origin = chip_from(k) * ntp + lax.rem(c + ntp - m, ntp)
                partner(
                    own, view(origin), psend.at[m, base + k], precv.at[m, base + k], m
                ).wait_recv()
                consume(origin)

    def own_chip(own, view, sems, base, consume):
        send, recv, psend, precv = sems
        for m in range(1, ntp):
            origin = f * ntp + lax.rem(c + ntp - m, ntp)
            partner(own, view(origin), psend.at[m, base], precv.at[m, base], m).wait_recv()
            consume(origin)

    def send_shift(d, carry):
        pltpu.make_async_remote_copy(
            src_ref=shbuf.at[0],
            dst_ref=shbuf.at[d],
            send_sem=sh_send.at[d],
            recv_sem=sh_recv.at[d],
            device_id={"sp": s + d},
            device_id_type=MESH,
        ).start()
        return carry

    def project(index, row0, first):
        rs = pl.ds(row0, KEY_TILE)
        x = xbuf[index, rs, :].astype(F32)
        per = cols // LANES
        gain = jnp.concatenate(
            [in_gain[pl.ds(index * per + j, 1), :] for j in range(per)], axis=1
        )
        scaled = (x * gain).astype(BF16)
        w = wbuf[pl.ds(pl.multiple_of(index * cols, cols), cols), :]
        part = jnp.dot(scaled, w, preferred_element_type=F32)
        sq = x * x
        folded = sq[:, :LANES]
        for j in range(1, per):
            folded = folded + sq[:, j * LANES : (j + 1) * LANES]
        if first:
            acc[rs, :] = part
            squares[rs, :] = folded
        else:
            acc[rs, :] += part
            squares[rs, :] += folded

    def kv_copy(d, t):
        rs = pl.ds(t * KEY_TILE, KEY_TILE)
        return pltpu.make_async_remote_copy(
            src_ref=kvbuf.at[0, rs],
            dst_ref=kvbuf.at[d, rs],
            send_sem=kv_send.at[d, t],
            recv_sem=kv_recv.at[d, t],
            device_id={"sp": lax.rem(s + d, nsp)},
            device_id_type=MESH,
        )

    def sh_copy(d):
        return pltpu.make_async_remote_copy(
            src_ref=shbuf.at[0],
            dst_ref=shbuf.at[d],
            send_sem=sh_send.at[d],
            recv_sem=sh_recv.at[d],
            device_id={"sp": lax.rem(s + d, nsp)},
            device_id_type=MESH,
        )

    halo = pltpu.make_async_remote_copy(
        src_ref=gbuf.at[pl.ds(rows, HALO)],
        dst_ref=gbuf.at[pl.ds(0, HALO)],
        send_sem=halo_sem.at[0],
        recv_sem=halo_sem.at[1],
        device_id={"sp": lax.rem(s + 1, nsp)},
        device_id_type=MESH,
    )

    lane = lax.broadcasted_iota(jnp.int32, (1, width), 1)
    head_lanes = [
        ((lane >= h * HEAD_DIM) & (lane < (h + 1) * HEAD_DIM)).astype(F32) for h in range(heads)
    ]
    tiles = rows // KEY_TILE
    tok_sems = (tok_send, tok_recv, tokp_send, tokp_recv)
    order = list(range(tiles - 1, -1, -1))

    def own_rows(t):
        return tokens.at[pl.ds(t * KEY_TILE, KEY_TILE)]

    def token_view(t):
        return lambda index: xbuf.at[index, pl.ds(t * KEY_TILE, KEY_TILE)]

    for t in order:
        start(own_rows(t), token_view(t), tok_sems, t * nfs)
    lax.fori_loop(1, nsp - s, send_shift, 0)
    for copy in locals_[:6]:
        copy.wait()

    for t in order:
        row0 = t * KEY_TILE
        rs = pl.ds(row0, KEY_TILE)
        args = (own_rows(t), token_view(t), tok_sems, t * nfs)

        def consume(index, row0=row0):
            project(index, row0, False)

        project(g, row0, True)
        own_chip(*args, consume)
        relay(*args, consume)
        finish_relay(*args, consume)
        scale = lax.rsqrt(jnp.sum(squares[rs, :], axis=1, keepdims=True) / model + epsilon)

        def projected(i, rs=rs, scale=scale):
            return (acc[rs, i * width : (i + 1) * width] * scale).astype(BF16)

        kvbuf[0, rs, :width] = projected(3)
        kvbuf[0, rs, width:] = projected(4)
        a = projected(0).astype(F32)
        gate = projected(1).astype(F32)
        gbuf[pl.ds(HALO + row0, KEY_TILE), :] = a / (1.0 + jnp.exp(-gate))
        if t == tiles - 1:

            @pl.when(s + 1 < nsp)
            def _():
                halo.start()

        def send_kv(d, carry, t=t):
            kv_copy(d, t).start()
            return carry

        lax.fori_loop(1, nsp - s, send_kv, 0)
        q = projected(2).astype(F32) * (HEAD_DIM**-0.5)
        for h in range(heads):
            qbuf[h, rs, :] = (q * head_lanes[h]).astype(BF16)
    obuf[...] = jnp.zeros_like(obuf)
    behind[...] = jnp.zeros_like(behind)

    def tile(slot, h, row0, count, key0, masked):
        rs = pl.ds(row0, count)
        keys = kvbuf[slot, pl.ds(key0, KEY_TILE), :width]
        values = kvbuf[slot, pl.ds(key0, KEY_TILE), width:]
        values = (values.astype(F32) * head_lanes[h]).astype(BF16)
        shifts = shbuf[slot, pl.ds(h, 1), pl.ds(key0, KEY_TILE)]
        scores = dot_tt(qbuf[h, rs, :], keys) * LOG2E + shifts
        fail = jnp.maximum(scores, 0.0) + LOG2E * jnp.log(1.0 + jnp.exp2(-jnp.abs(scores)))
        if masked:
            qi = row0 + lax.broadcasted_iota(jnp.int32, (count, KEY_TILE), 0)
            kk = key0 + lax.broadcasted_iota(jnp.int32, (count, KEY_TILE), 1)
            allowed = kk < qi
            fail = jnp.where(allowed, fail, 0.0)
        high = fail.astype(BF16)
        low = (fail - high.astype(F32)).astype(BF16)
        sums = jnp.dot(high, tri[...], preferred_element_type=F32) + jnp.dot(
            low, tri[...], preferred_element_type=F32
        )
        past = behind[h, rs, :]
        past_wide = jnp.concatenate([past] * (KEY_TILE // LANES), axis=1)
        weights = jnp.exp2(scores - sums - past_wide)
        if masked:
            weights = jnp.where(allowed, weights, 0.0)
        obuf[rs, :] += jnp.dot(weights.astype(BF16), values, preferred_element_type=F32)
        behind[h, rs, :] = past + sums[:, :1]

    for h in range(heads):
        for qt in range(tiles):
            for kt in range(qt, -1, -1):
                tile(0, h, qt * KEY_TILE, KEY_TILE, kt * KEY_TILE, kt == qt)

    @pl.when(s == 0)
    def _():
        gbuf[pl.ds(0, HALO), :] = jnp.zeros((HALO, width), F32)

    @pl.when(s > 0)
    def _():
        halo.wait_recv()

    ntaps = taps.shape[0]
    tap = taps[:, pl.ds(pl.multiple_of(g * width, width), width)].astype(F32)
    chunk = 128
    for r0 in range(0, rows, chunk):
        total = jnp.zeros((chunk, width), F32)
        for j in range(ntaps):
            first = r0 + j + HALO - (ntaps - 1)
            total = total + tap[j : j + 1, :] * gbuf[pl.ds(first, chunk), :]
        convbuf[pl.ds(r0, chunk), :] = total

    conv = convbuf[...]
    ones = jnp.ones((8, width), F32)
    sub = lax.broadcasted_iota(jnp.int32, (8, rows), 0)
    hp = lax.Precision.HIGHEST
    stat[0] = jnp.where(sub == 0, dot_tt(ones, conv, hp), dot_tt(ones, conv * conv, hp))

    def stat_copy(d):
        return pltpu.make_async_remote_copy(
            src_ref=stat.at[0],
            dst_ref=stat.at[d],
            send_sem=stat_send.at[d],
            recv_sem=stat_recv.at[d],
            device_id=in_group(lax.rem(g + d, group)),
            device_id_type=MESH,
        )

    for d in range(1, group):
        stat_copy(d).start()
    totals = stat[0]
    for d in range(1, group):
        stat_copy(d).wait_recv()
        totals = totals + stat[d]
    pick = lax.broadcasted_iota(jnp.int32, (8, width), 0)
    turned = (((0,), (0,)), ((), ()))
    first_sum = lax.dot_general(
        totals, (pick == 0).astype(F32), turned, precision=hp, preferred_element_type=F32
    )
    second_sum = lax.dot_general(
        totals, (pick == 1).astype(F32), turned, precision=hp, preferred_element_type=F32
    )
    mean = first_sum / channels
    spread = jnp.maximum(second_sum / channels - mean * mean, 0.0)
    normed = (conv - mean) * lax.rsqrt(spread + epsilon) * norm_gain[pl.ds(g, 1), :]
    mixed = (normed / (1.0 + jnp.exp(-normed))).astype(BF16)
    own_conv[...] = mixed
    cbuf[g] = mixed

    conv_args = (own_conv, lambda index: cbuf.at[index], (conv_send, conv_recv, convp_send, convp_recv), 0)
    start(*conv_args)

    def attend(d, carry):
        sh_copy(d).wait_recv()
        for kt in order:
            kv_copy(d, kt).wait_recv()
            for h in range(heads):
                tile(d, h, 0, rows, kt * KEY_TILE, False)
        return carry

    lax.fori_loop(1, s, attend, 0)
    relay(*conv_args, None)
    lax.fori_loop(jnp.maximum(s, 1), s + 1, attend, 0)

    attn = obuf[...].astype(BF16)
    own_attn[...] = attn
    abuf[g] = attn

    attn_args = (own_attn, lambda index: abuf.at[index], (att_send, att_recv, attp_send, attp_recv), 0)
    start(*attn_args)
    locals_[6].wait()

    def mix(buf, gain, base, index, first):
        v = buf[index].astype(F32)
        scaled = (v * gain[pl.ds(index, 1), :]).astype(BF16)
        w = wout[pl.ds(pl.multiple_of(base + index * width, width), width), :]
        part = jnp.dot(scaled, w, preferred_element_type=F32)
        if first:
            acc[:, : out.shape[1]] = part
            squares[...] = v * v
        else:
            acc[:, : out.shape[1]] += part
            squares[...] += v * v

    def mix_conv(index):
        mix(cbuf, conv_gain, 0, index, False)

    def mix_attn(index):
        mix(abuf, attn_gain, channels, index, False)

    out_width = out.shape[1]
    mix(cbuf, conv_gain, 0, g, True)
    own_chip(*conv_args, mix_conv)
    for k in range(1, nfs):
        mix_conv(chip_from(k) * ntp + c)
    finish_relay(*conv_args, mix_conv)
    conv_scale = lax.rsqrt(jnp.sum(squares[...], axis=1, keepdims=True) / channels + epsilon)
    acc[:, out_width : 2 * out_width] = acc[:, :out_width] * conv_scale
    mix(abuf, attn_gain, channels, g, True)
    own_chip(*attn_args, mix_attn)
    relay(*attn_args, mix_attn)
    finish_relay(*attn_args, mix_attn)
    attn_scale = lax.rsqrt(jnp.sum(squares[...], axis=1, keepdims=True) / channels + epsilon)
    out[...] = (acc[:, out_width : 2 * out_width] + acc[:, :out_width] * attn_scale).astype(BF16)

    for copy in sent:
        copy.wait_send()
    for d in range(1, group):
        stat_copy(d).wait_send()

    @pl.when(s + 1 < nsp)
    def _():
        halo.wait_send()

    def finish(d, carry):
        sh_copy(d).wait_send()
        for t in range(tiles):
            kv_copy(d, t).wait_send()
        return carry

    lax.fori_loop(1, nsp - s, finish, 0)


def per_device(
    tokens,
    in_gain,
    conv_a_weight,
    conv_gate_weight,
    query_weight,
    key_weight,
    value_weight,
    conv_taps,
    conv_norm_gain,
    break_shift,
    conv_out_gain,
    attn_out_gain,
    out_weight,
):
    nsp, nfs, ntp = (lax.axis_size(axis) for axis in ("sp", "fs", "tp"))
    group = nfs * ntp
    rows, cols = tokens.shape
    model = in_gain.shape[0]
    width = conv_a_weight.shape[1]
    heads = break_shift.shape[0]
    out_width = out_weight.shape[1]
    tiles = rows // KEY_TILE
    vm = pl.BlockSpec(memory_space=pltpu.VMEM)
    hbm = pl.BlockSpec(memory_space=pl.ANY)
    dma = pltpu.SemaphoreType.DMA
    return pl.pallas_call(
        functools.partial(layer_kernel, nsp, nfs, ntp),
        out_shape=jax.ShapeDtypeStruct((rows, out_width), BF16),
        in_specs=[hbm] * 7 + [vm] * 6,
        out_specs=vm,
        scratch_shapes=[
            pltpu.VMEM((group, rows, cols), BF16),
            pltpu.VMEM((model, 5 * width), BF16),
            pltpu.VMEM((model, out_width), BF16),
            pltpu.VMEM((rows, 5 * width), F32),
            pltpu.VMEM((rows, LANES), F32),
            pltpu.VMEM((heads, rows, width), BF16),
            pltpu.VMEM((nsp, rows, 2 * width), BF16),
            pltpu.VMEM((nsp, 8, rows), F32),
            pltpu.VMEM((HALO + rows, width), F32),
            pltpu.VMEM((rows, width), F32),
            pltpu.VMEM((KEY_TILE, KEY_TILE), BF16),
            pltpu.VMEM((group, 8, rows), F32),
            pltpu.VMEM((rows, width), BF16),
            pltpu.VMEM((rows, width), BF16),
            pltpu.VMEM((group, rows, width), BF16),
            pltpu.VMEM((group, rows, width), BF16),
            pltpu.VMEM((rows, width), F32),
            pltpu.VMEM((heads, rows, LANES), F32),
            dma((7,)),
            dma((tiles * nfs,)),
            dma((tiles * nfs,)),
            dma((ntp, tiles * nfs)),
            dma((ntp, tiles * nfs)),
            dma((nfs,)),
            dma((nfs,)),
            dma((ntp, nfs)),
            dma((ntp, nfs)),
            dma((nsp, tiles)),
            dma((nsp, tiles)),
            dma((nsp,)),
            dma((nsp,)),
            dma((2,)),
            dma((group,)),
            dma((group,)),
            dma((nfs,)),
            dma((nfs,)),
            dma((ntp, nfs)),
            dma((ntp, nfs)),
        ],
        compiler_params=pltpu.CompilerParams(
            collective_id=0, has_side_effects=True, vmem_limit_bytes=67043328
        ),
        name="layer",
    )(
        tokens,
        conv_a_weight,
        conv_gate_weight,
        query_weight,
        key_weight,
        value_weight,
        out_weight,
        in_gain.reshape(-1, LANES),
        conv_taps,
        conv_norm_gain.reshape(-1, LANES),
        break_shift,
        conv_out_gain.reshape(-1, LANES),
        attn_out_gain.reshape(-1, LANES),
    )


def solution(mesh):
    split = P(None, ("fs", "tp"))
    return jax.shard_map(
        per_device,
        mesh=mesh,
        in_specs=(
            P("sp", ("fs", "tp")),
            P(),
            split,
            split,
            split,
            split,
            split,
            P(),
            P(),
            P(("fs", "tp"), "sp"),
            P(),
            P(),
            split,
        ),
        out_specs=P("sp", ("fs", "tp")),
        check_vma=False,
    )
```

```python
import functools
import math

import jax
import jax.numpy as jnp
from jax import lax
from jax.experimental import pallas as pl
from jax.experimental.pallas import tpu as pltpu
from jax.sharding import PartitionSpec as P

HEAD_DIM = 64
LANES = 128
KEY_TILE = 256
HALO = 32
LOG2E = math.log2(math.e)
MESH = pl.DeviceIdType.MESH
F32 = jnp.float32
BF16 = jnp.bfloat16

epsilon = 1e-06


def dot_tt(left, right, precision=None):
    return lax.dot_general(
        left, right, (((1,), (1,)), ((), ())), precision=precision, preferred_element_type=F32
    )


def layer_kernel(
    nsp,
    nfs,
    ntp,
    tokens,
    w_a,
    w_gate,
    w_q,
    w_k,
    w_v,
    w_out,
    in_gain,
    taps,
    norm_gain,
    shift,
    conv_gain,
    attn_gain,
    out,
    xbuf,
    wbuf,
    wout,
    acc,
    squares,
    qbuf,
    kvbuf,
    shbuf,
    gbuf,
    convbuf,
    tri,
    stat,
    own_conv,
    own_attn,
    cbuf,
    abuf,
    obuf,
    behind,
    local_sem,
    tok_send,
    tok_recv,
    tokp_send,
    tokp_recv,
    att_send,
    att_recv,
    attp_send,
    attp_recv,
    kv_send,
    kv_recv,
    sh_send,
    sh_recv,
    halo_sem,
    stat_send,
    stat_recv,
    conv_send,
    conv_recv,
    convp_send,
    convp_recv,
):
    s = lax.axis_index("sp")
    f = lax.axis_index("fs")
    c = lax.axis_index("tp")
    group = nfs * ntp
    g = f * ntp + c
    rows = tokens.shape[0]
    cols = tokens.shape[1]
    width = w_a.shape[1]
    heads = shift.shape[0]
    channels = width * group
    model = cols * group

    def in_group(index):
        return {"fs": index // ntp, "tp": lax.rem(index, ntp)}

    barrier = pltpu.get_barrier_semaphore()
    for d in range(1, group):
        pl.semaphore_signal(
            barrier, inc=1, device_id=in_group(lax.rem(g + d, group)), device_id_type=MESH
        )

    def greet(d, carry):
        pl.semaphore_signal(
            barrier, inc=1, device_id={"sp": lax.rem(s + d, nsp)}, device_id_type=MESH
        )
        return carry

    lax.fori_loop(1, nsp, greet, 0)

    locals_ = [pltpu.make_async_copy(tokens, xbuf.at[g], local_sem.at[0])]
    for i, w in enumerate((w_a, w_gate, w_q, w_k, w_v)):
        locals_.append(
            pltpu.make_async_copy(
                w, wbuf.at[:, pl.ds(i * width, width)], local_sem.at[1 + i]
            )
        )
    locals_.append(pltpu.make_async_copy(w_out, wout, local_sem.at[6]))
    for copy in locals_:
        copy.start()

    shbuf[0] = jnp.zeros(shbuf.shape[1:], F32)
    shbuf[0, pl.ds(0, heads), :] = shift[...].astype(F32) * LOG2E
    ki = lax.broadcasted_iota(jnp.int32, (KEY_TILE, KEY_TILE), 0)
    kj = lax.broadcasted_iota(jnp.int32, (KEY_TILE, KEY_TILE), 1)
    tri[...] = (ki >= kj).astype(F32).astype(BF16)

    pl.semaphore_wait(barrier, group - 1 + nsp - 1)

    def direct(src, dst, send, recv, k):
        return pltpu.make_async_remote_copy(
            src_ref=src,
            dst_ref=dst,
            send_sem=send,
            recv_sem=recv,
            device_id={"fs": lax.rem(f + k, nfs)},
            device_id_type=MESH,
        )

    def partner(src, dst, send, recv, m):
        return pltpu.make_async_remote_copy(
            src_ref=src,
            dst_ref=dst,
            send_sem=send,
            recv_sem=recv,
            device_id={"tp": lax.rem(c + m, ntp)},
            device_id_type=MESH,
        )

    def chip_from(k):
        return lax.rem(f + nfs - k, nfs)

    sent = []

    def start(own, view, sems, base):
        send, recv, psend, precv = sems
        for k in range(1, nfs):
            copy = direct(own, view(g), send.at[base + k], recv.at[base + k], k)
            copy.start()
            sent.append(copy)
        for m in range(1, ntp):
            copy = partner(own, view(g), psend.at[m, base], precv.at[m, base], m)
            copy.start()
            sent.append(copy)

    def relay(own, view, sems, base, consume):
        send, recv, psend, precv = sems
        for k in range(1, nfs):
            origin = chip_from(k) * ntp + c
            direct(own, view(origin), send.at[base + k], recv.at[base + k], k).wait_recv()
            for m in range(1, ntp):
                copy = partner(
                    view(origin), view(origin), psend.at[m, base + k], precv.at[m, base + k], m
                )
                copy.start()
                sent.append(copy)
            if consume is not None:
                consume(origin)

    def finish_relay(own, view, sems, base, consume):
        send, recv, psend, precv = sems
        for k in range(1, nfs):
            for m in range(1, ntp):
                origin = chip_from(k) * ntp + lax.rem(c + ntp - m, ntp)
                partner(
                    own, view(origin), psend.at[m, base + k], precv.at[m, base + k], m
                ).wait_recv()
                consume(origin)

    def own_chip(own, view, sems, base, consume):
        send, recv, psend, precv = sems
        for m in range(1, ntp):
            origin = f * ntp + lax.rem(c + ntp - m, ntp)
            partner(own, view(origin), psend.at[m, base], precv.at[m, base], m).wait_recv()
            consume(origin)

    def send_shift(d, carry):
        pltpu.make_async_remote_copy(
            src_ref=shbuf.at[0],
            dst_ref=shbuf.at[d],
            send_sem=sh_send.at[d],
            recv_sem=sh_recv.at[d],
            device_id={"sp": s + d},
            device_id_type=MESH,
        ).start()
        return carry

    def project(index, row0, first):
        rs = pl.ds(row0, KEY_TILE)
        x = xbuf[index, rs, :].astype(F32)
        per = cols // LANES
        gain = jnp.concatenate(
            [in_gain[pl.ds(index * per + j, 1), :] for j in range(per)], axis=1
        )
        scaled = (x * gain).astype(BF16)
        w = wbuf[pl.ds(pl.multiple_of(index * cols, cols), cols), :]
        part = jnp.dot(scaled, w, preferred_element_type=F32)
        sq = x * x
        folded = sq[:, :LANES]
        for j in range(1, per):
            folded = folded + sq[:, j * LANES : (j + 1) * LANES]
        if first:
            acc[rs, :] = part
            squares[rs, :] = folded
        else:
            acc[rs, :] += part
            squares[rs, :] += folded

    def kv_copy(d, t):
        rs = pl.ds(t * KEY_TILE, KEY_TILE)
        return pltpu.make_async_remote_copy(
            src_ref=kvbuf.at[0, rs],
            dst_ref=kvbuf.at[d, rs],
            send_sem=kv_send.at[d, t],
            recv_sem=kv_recv.at[d, t],
            device_id={"sp": lax.rem(s + d, nsp)},
            device_id_type=MESH,
        )

    def sh_copy(d):
        return pltpu.make_async_remote_copy(
            src_ref=shbuf.at[0],
            dst_ref=shbuf.at[d],
            send_sem=sh_send.at[d],
            recv_sem=sh_recv.at[d],
            device_id={"sp": lax.rem(s + d, nsp)},
            device_id_type=MESH,
        )

    halo = pltpu.make_async_remote_copy(
        src_ref=gbuf.at[pl.ds(rows, HALO)],
        dst_ref=gbuf.at[pl.ds(0, HALO)],
        send_sem=halo_sem.at[0],
        recv_sem=halo_sem.at[1],
        device_id={"sp": lax.rem(s + 1, nsp)},
        device_id_type=MESH,
    )

    lane = lax.broadcasted_iota(jnp.int32, (1, width), 1)
    head_lanes = [
        ((lane >= h * HEAD_DIM) & (lane < (h + 1) * HEAD_DIM)).astype(F32) for h in range(heads)
    ]
    tiles = rows // KEY_TILE
    tok_sems = (tok_send, tok_recv, tokp_send, tokp_recv)
    order = list(range(tiles - 1, -1, -1))

    def own_rows(t):
        return tokens.at[pl.ds(t * KEY_TILE, KEY_TILE)]

    def token_view(t):
        return lambda index: xbuf.at[index, pl.ds(t * KEY_TILE, KEY_TILE)]

    for t in order:
        start(own_rows(t), token_view(t), tok_sems, t * nfs)
    lax.fori_loop(1, nsp - s, send_shift, 0)
    for copy in locals_[:6]:
        copy.wait()

    for t in order:
        row0 = t * KEY_TILE
        rs = pl.ds(row0, KEY_TILE)
        args = (own_rows(t), token_view(t), tok_sems, t * nfs)

        def consume(index, row0=row0):
            project(index, row0, False)

        project(g, row0, True)
        own_chip(*args, consume)
        relay(*args, consume)
        finish_relay(*args, consume)
        scale = lax.rsqrt(jnp.sum(squares[rs, :], axis=1, keepdims=True) / model + epsilon)

        def projected(i, rs=rs, scale=scale):
            return (acc[rs, i * width : (i + 1) * width] * scale).astype(BF16)

        kvbuf[0, rs, :width] = projected(3)
        kvbuf[0, rs, width:] = projected(4)
        a = projected(0).astype(F32)
        gate = projected(1).astype(F32)
        gbuf[pl.ds(HALO + row0, KEY_TILE), :] = a / (1.0 + jnp.exp(-gate))
        if t == tiles - 1:

            @pl.when(s + 1 < nsp)
            def _():
                halo.start()

        def send_kv(d, carry, t=t):
            kv_copy(d, t).start()
            return carry

        lax.fori_loop(1, nsp - s, send_kv, 0)
        q = projected(2).astype(F32) * (HEAD_DIM**-0.5)
        for h in range(heads):
            qbuf[h, rs, :] = (q * head_lanes[h]).astype(BF16)
    obuf[...] = jnp.zeros_like(obuf)
    behind[...] = jnp.zeros_like(behind)

    def tile(slot, h, row0, count, key0, masked):
        rs = pl.ds(row0, count)
        keys = kvbuf[slot, pl.ds(key0, KEY_TILE), :width]
        values = kvbuf[slot, pl.ds(key0, KEY_TILE), width:]
        values = (values.astype(F32) * head_lanes[h]).astype(BF16)
        shifts = shbuf[slot, pl.ds(h, 1), pl.ds(key0, KEY_TILE)]
        scores = dot_tt(qbuf[h, rs, :], keys) * LOG2E + shifts
        fail = jnp.maximum(scores, 0.0) + LOG2E * jnp.log(1.0 + jnp.exp2(-jnp.abs(scores)))
        if masked:
            qi = row0 + lax.broadcasted_iota(jnp.int32, (count, KEY_TILE), 0)
            kk = key0 + lax.broadcasted_iota(jnp.int32, (count, KEY_TILE), 1)
            allowed = kk < qi
            fail = jnp.where(allowed, fail, 0.0)
        high = fail.astype(BF16)
        low = (fail - high.astype(F32)).astype(BF16)
        sums = jnp.dot(high, tri[...], preferred_element_type=F32) + jnp.dot(
            low, tri[...], preferred_element_type=F32
        )
        past = behind[h, rs, :]
        past_wide = jnp.concatenate([past] * (KEY_TILE // LANES), axis=1)
        weights = jnp.exp2(scores - sums - past_wide)
        if masked:
            weights = jnp.where(allowed, weights, 0.0)
        obuf[rs, :] += jnp.dot(weights.astype(BF16), values, preferred_element_type=F32)
        behind[h, rs, :] = past + sums[:, :1]

    for h in range(heads):
        for qt in range(tiles):
            for kt in range(qt, -1, -1):
                tile(0, h, qt * KEY_TILE, KEY_TILE, kt * KEY_TILE, kt == qt)

    @pl.when(s == 0)
    def _():
        gbuf[pl.ds(0, HALO), :] = jnp.zeros((HALO, width), F32)

    @pl.when(s > 0)
    def _():
        halo.wait_recv()

    ntaps = taps.shape[0]
    tap = taps[:, pl.ds(pl.multiple_of(g * width, width), width)].astype(F32)
    chunk = 128
    for r0 in range(0, rows, chunk):
        total = jnp.zeros((chunk, width), F32)
        for j in range(ntaps):
            first = r0 + j + HALO - (ntaps - 1)
            total = total + tap[j : j + 1, :] * gbuf[pl.ds(first, chunk), :]
        convbuf[pl.ds(r0, chunk), :] = total

    conv = convbuf[...]
    ones = jnp.ones((8, width), F32)
    sub = lax.broadcasted_iota(jnp.int32, (8, rows), 0)
    hp = lax.Precision.HIGHEST
    stat[0] = jnp.where(sub == 0, dot_tt(ones, conv, hp), dot_tt(ones, conv * conv, hp))

    def stat_copy(d):
        return pltpu.make_async_remote_copy(
            src_ref=stat.at[0],
            dst_ref=stat.at[d],
            send_sem=stat_send.at[d],
            recv_sem=stat_recv.at[d],
            device_id=in_group(lax.rem(g + d, group)),
            device_id_type=MESH,
        )

    for d in range(1, group):
        stat_copy(d).start()
    totals = stat[0]
    for d in range(1, group):
        stat_copy(d).wait_recv()
        totals = totals + stat[d]
    pick = lax.broadcasted_iota(jnp.int32, (8, width), 0)
    turned = (((0,), (0,)), ((), ()))
    first_sum = lax.dot_general(
        totals, (pick == 0).astype(F32), turned, precision=hp, preferred_element_type=F32
    )
    second_sum = lax.dot_general(
        totals, (pick == 1).astype(F32), turned, precision=hp, preferred_element_type=F32
    )
    mean = first_sum / channels
    spread = jnp.maximum(second_sum / channels - mean * mean, 0.0)
    normed = (conv - mean) * lax.rsqrt(spread + epsilon) * norm_gain[pl.ds(g, 1), :]
    mixed = (normed / (1.0 + jnp.exp(-normed))).astype(BF16)
    own_conv[...] = mixed
    cbuf[g] = mixed

    conv_args = (own_conv, lambda index: cbuf.at[index], (conv_send, conv_recv, convp_send, convp_recv), 0)
    start(*conv_args)

    def attend(d, carry):
        sh_copy(d).wait_recv()
        for kt in order:
            kv_copy(d, kt).wait_recv()
            for h in range(heads):
                tile(d, h, 0, rows, kt * KEY_TILE, False)
        return carry

    lax.fori_loop(1, s, attend, 0)
    relay(*conv_args, None)
    att_sems = (att_send, att_recv, attp_send, attp_recv)

    def attn_rows(t):
        return own_attn.at[pl.ds(t * KEY_TILE, KEY_TILE)]

    def attn_view(t):
        return lambda index: abuf.at[index, pl.ds(t * KEY_TILE, KEY_TILE)]

    for qt in order:

        def attend_part(d, carry, qt=qt):
            if qt == order[0]:
                sh_copy(d).wait_recv()
            for kt in order:
                if qt == order[0]:
                    kv_copy(d, kt).wait_recv()
                for h in range(heads):
                    tile(d, h, qt * KEY_TILE, KEY_TILE, kt * KEY_TILE, False)
            return carry

        lax.fori_loop(jnp.maximum(s, 1), s + 1, attend_part, 0)
        rs = pl.ds(qt * KEY_TILE, KEY_TILE)
        attn = obuf[rs, :].astype(BF16)
        own_attn[rs, :] = attn
        abuf[g, rs, :] = attn
        start(attn_rows(qt), attn_view(qt), att_sems, qt * nfs)
    locals_[6].wait()

    def mix_attn(index, row0, first):
        rs = pl.ds(row0, KEY_TILE)
        v = abuf[index, rs, :].astype(F32)
        scaled = (v * attn_gain[pl.ds(index, 1), :]).astype(BF16)
        w = wout[pl.ds(pl.multiple_of(channels + index * width, width), width), :]
        part = jnp.dot(scaled, w, preferred_element_type=F32)
        if first:
            acc[rs, :out_width] = part
            squares[rs, :] = v * v
        else:
            acc[rs, :out_width] += part
            squares[rs, :] += v * v

    def nothing(index):
        return None

    out_width = out.shape[1]
    own_chip(*conv_args, nothing)
    finish_relay(*conv_args, nothing)
    for t in order:
        rs = pl.ds(t * KEY_TILE, KEY_TILE)
        pieces = []
        folded = jnp.zeros((KEY_TILE, width), F32)
        for index in range(group):
            v = cbuf[index, rs, :].astype(F32)
            folded = folded + v * v
            pieces.append((v * conv_gain[index : index + 1, :]).astype(BF16))
        product = jnp.dot(
            jnp.concatenate(pieces, axis=1), wout[:channels, :], preferred_element_type=F32
        )
        conv_scale = lax.rsqrt(jnp.sum(folded, axis=1, keepdims=True) / channels + epsilon)
        acc[rs, out_width : 2 * out_width] = product * conv_scale
    for t in order:
        row0 = t * KEY_TILE
        rs = pl.ds(row0, KEY_TILE)
        args = (attn_rows(t), attn_view(t), att_sems, t * nfs)

        def consume_attn(index, row0=row0):
            mix_attn(index, row0, False)

        mix_attn(g, row0, True)
        own_chip(*args, consume_attn)
        relay(*args, consume_attn)
        finish_relay(*args, consume_attn)
        attn_scale = lax.rsqrt(
            jnp.sum(squares[rs, :], axis=1, keepdims=True) / channels + epsilon
        )
        out[rs, :] = (
            acc[rs, out_width : 2 * out_width] + acc[rs, :out_width] * attn_scale
        ).astype(BF16)

    for copy in sent:
        copy.wait_send()
    for d in range(1, group):
        stat_copy(d).wait_send()

    @pl.when(s + 1 < nsp)
    def _():
        halo.wait_send()

    def finish(d, carry):
        sh_copy(d).wait_send()
        for t in range(tiles):
            kv_copy(d, t).wait_send()
        return carry

    lax.fori_loop(1, nsp - s, finish, 0)


def per_device(
    tokens,
    in_gain,
    conv_a_weight,
    conv_gate_weight,
    query_weight,
    key_weight,
    value_weight,
    conv_taps,
    conv_norm_gain,
    break_shift,
    conv_out_gain,
    attn_out_gain,
    out_weight,
):
    nsp, nfs, ntp = (lax.axis_size(axis) for axis in ("sp", "fs", "tp"))
    group = nfs * ntp
    rows, cols = tokens.shape
    model = in_gain.shape[0]
    width = conv_a_weight.shape[1]
    heads = break_shift.shape[0]
    out_width = out_weight.shape[1]
    tiles = rows // KEY_TILE
    vm = pl.BlockSpec(memory_space=pltpu.VMEM)
    hbm = pl.BlockSpec(memory_space=pl.ANY)
    dma = pltpu.SemaphoreType.DMA
    return pl.pallas_call(
        functools.partial(layer_kernel, nsp, nfs, ntp),
        out_shape=jax.ShapeDtypeStruct((rows, out_width), BF16),
        in_specs=[hbm] * 7 + [vm] * 6,
        out_specs=vm,
        scratch_shapes=[
            pltpu.VMEM((group, rows, cols), BF16),
            pltpu.VMEM((model, 5 * width), BF16),
            pltpu.VMEM((model, out_width), BF16),
            pltpu.VMEM((rows, 5 * width), F32),
            pltpu.VMEM((rows, LANES), F32),
            pltpu.VMEM((heads, rows, width), BF16),
            pltpu.VMEM((nsp, rows, 2 * width), BF16),
            pltpu.VMEM((nsp, 8, rows), F32),
            pltpu.VMEM((HALO + rows, width), F32),
            pltpu.VMEM((rows, width), F32),
            pltpu.VMEM((KEY_TILE, KEY_TILE), BF16),
            pltpu.VMEM((group, 8, rows), F32),
            pltpu.VMEM((rows, width), BF16),
            pltpu.VMEM((rows, width), BF16),
            pltpu.VMEM((group, rows, width), BF16),
            pltpu.VMEM((group, rows, width), BF16),
            pltpu.VMEM((rows, width), F32),
            pltpu.VMEM((heads, rows, LANES), F32),
            dma((7,)),
            dma((tiles * nfs,)),
            dma((tiles * nfs,)),
            dma((ntp, tiles * nfs)),
            dma((ntp, tiles * nfs)),
            dma((tiles * nfs,)),
            dma((tiles * nfs,)),
            dma((ntp, tiles * nfs)),
            dma((ntp, tiles * nfs)),
            dma((nsp, tiles)),
            dma((nsp, tiles)),
            dma((nsp,)),
            dma((nsp,)),
            dma((2,)),
            dma((group,)),
            dma((group,)),
            dma((nfs,)),
            dma((nfs,)),
            dma((ntp, nfs)),
            dma((ntp, nfs)),
        ],
        compiler_params=pltpu.CompilerParams(
            collective_id=0, has_side_effects=True, vmem_limit_bytes=67043328
        ),
        name="layer",
    )(
        tokens,
        conv_a_weight,
        conv_gate_weight,
        query_weight,
        key_weight,
        value_weight,
        out_weight,
        in_gain.reshape(-1, LANES),
        conv_taps,
        conv_norm_gain.reshape(-1, LANES),
        break_shift,
        conv_out_gain.reshape(-1, LANES),
        attn_out_gain.reshape(-1, LANES),
    )


def solution(mesh):
    split = P(None, ("fs", "tp"))
    return jax.shard_map(
        per_device,
        mesh=mesh,
        in_specs=(
            P("sp", ("fs", "tp")),
            P(),
            split,
            split,
            split,
            split,
            split,
            P(),
            P(),
            P(("fs", "tp"), "sp"),
            P(),
            P(),
            split,
        ),
        out_specs=P("sp", ("fs", "tp")),
        check_vma=False,
    )
```
